256 devices in a mesh: ep: 16 (over y, x), tp: 16 (over z, core).
Axes of the slice: x: 4, y: 4, z: 8, core: 2. Of those that a mesh axis runs over, the one named last changes fastest.
Arguments:
- tokens: bfloat16 [256, 2048], P('ep', 'tp'), may hold values from -6 to 6
- key_cache: bfloat16 [256, 16, 1024, 128], P('ep', 'tp'), may hold values from -1700 to 1700
- value_cache: bfloat16 [256, 16, 1024, 128], P('ep', 'tp'), may hold values from -6 to 6
- gate_totals: float32 [256, 16, 1024], P('ep', 'tp'), as said below
- lengths: int32 [256], P('ep'), may hold values from 128 to 1024
- attn_gain: float32 [2048], replicated, may hold values from 0.1 to 1.9
- w_query: bfloat16 [2048, 2048], P(None, 'tp'), may hold values from -0.125 to 0.125
- w_key: bfloat16 [2048, 2048], P(None, 'tp'), may hold values from -0.125 to 0.125
- w_value: bfloat16 [2048, 2048], P(None, 'tp'), may hold values from -0.125 to 0.125
- w_forget: bfloat16 [2048, 16], replicated, may hold values from -0.125 to 0.125
- forget_bias: float32 [16], replicated, may hold values from -3 to 0
- w_attn_out: bfloat16 [2048, 2048], P('tp'), may hold values from -0.1875 to 0.1875
- moe_gain: float32 [2048], replicated, may hold values from 0.1 to 1.9
- group_ids: int32 [256, 1], P('ep'), may hold values from 0 to 15; in each aligned block of 16 rows (0 to 15, 16 to 31, ...) at most 2 rows name the same one
- inner_ids: int32 [256, 2], P('ep'), may hold values from 0 to 3, all different within a row
- group_prob: float32 [256], P('ep'), may hold values from 0.2 to 1
- pair_logits: float32 [256, 2], P('ep'), may hold values from -6 to 6
- w_expert_gate: bfloat16 [16, 2048, 2048], P('ep', None, 'tp'), may hold values from -0.125 to 0.125
- w_expert_up: bfloat16 [16, 2048, 2048], P('ep', None, 'tp'), may hold values from -0.125 to 0.125
- w_expert_down: bfloat16 [16, 2048, 2048], P('ep', 'tp'), may hold values from -0.375 to 0.375
- w_dense_in: bfloat16 [2048, 2048], P(None, 'tp'), may hold values from -0.125 to 0.125
- w_dense_out: bfloat16 [2048, 2048], P('tp'), may hold values from -0.1875 to 0.1875
- dense_gate: float32 [2048], P('tp'), may hold values from -2 to 2
Outputs:
- layer_output: bfloat16 [256, 2048], P('ep', 'tp')
- new_keys: bfloat16 [256, 16, 128], P('ep', 'tp')
- new_values: bfloat16 [256, 16, 128], P('ep', 'tp')
- new_gates: float32 [256, 16], P('ep', 'tp')
The draws below stay inside these ranges and needn't reach their ends.
Inputs may be any that keep to these rules, and one draw needn't show every extreme that they name: `group_ids`: within the 16 sequences of each index of ep (aligned blocks of rows), no group is named by more than 2 sequences, a bound that some block reaches. `inner_ids`: each row names 2 different experts of its group. `gate_totals`: along positions the values of each sequence and head never rise.
All inputs are finite; a program needn't handle non-finite values.
Results may differ from the reference program's by a relative error of at most 0.011.
Values may be sent and summed in bfloat16 or wider, within the bound.
A program may use at most 64 MiB of HBM per device.

```python
import math
import jax
import jax.numpy as jnp
import numpy as np
from jax import lax

D = 2048
HEADS = 16
HEAD_DIM = 128
FFE = 512
EPG = 4
TOPK = 2
FFD = 2048
SEQ_GRP = 16
STORED_ENTRIES = 1024
STREAM_COUNT = 256
GROUPS = 16
CAP = 2
N_EP = 16


def draw_key_cache(key, part):
    full_shape = (STREAM_COUNT, HEADS, STORED_ENTRIES, HEAD_DIM)
    base_draw = jnp.clip(jax.random.normal(jax.random.fold_in(key, 11), full_shape, jnp.float32), -5.0, 5.0)
    return base_draw.astype(jnp.bfloat16)


def draw_gate_totals(key, part):
    noise_child_seeds = jax.random.split(jax.random.fold_in(key, 21), 7)
    slow_share = 0.5
    gradual_zone_flags = jax.random.uniform(noise_child_seeds[0], (1, HEADS, 1), jnp.float32) < slow_share
    slow_total = jax.random.uniform(noise_child_seeds[1], (STREAM_COUNT, HEADS, 1), jnp.float32, 0.2, 0.7)
    fast_span = jax.random.uniform(noise_child_seeds[2], (1, HEADS, 1), jnp.float32, 30.0, 100.0)
    seq_factor = jnp.exp(jax.random.uniform(noise_child_seeds[3], (STREAM_COUNT, 1, 1), jnp.float32, 0.0, math.log(2.0)))
    rough_mult = jax.random.uniform(noise_child_seeds[4], (STREAM_COUNT, HEADS, STORED_ENTRIES), jnp.float32, 0.5, 1.5)
    fading_per_tick = jnp.where(gradual_zone_flags, slow_total / STORED_ENTRIES, 1.0 / fast_span) * seq_factor * rough_mult
    spike_index_point = jax.random.randint(noise_child_seeds[5], (STREAM_COUNT, 1, 1, 2), 0, STORED_ENTRIES)
    entry_indices = jnp.arange(STORED_ENTRIES)[None, None, :, None]
    spike_zone_flags = jnp.any(entry_indices == spike_index_point, axis=-1)
    keeping_logarithm_multiplier = jnp.log(jax.random.uniform(noise_child_seeds[6], (STREAM_COUNT, HEADS, 1), jnp.float32, 0.55, 0.8))
    logarithm_fading_tick = -fading_per_tick + jnp.where(spike_zone_flags & gradual_zone_flags, keeping_logarithm_multiplier, 0.0)
    return jnp.cumsum(logarithm_fading_tick, axis=-1)


def set_ends(array, rng, low, top_value):
    extent = array.shape
    index_at = [jax.random.randint(jax.random.fold_in(rng, axis), (), 0, extent[axis]) for axis in range(len(extent))]
    array = array.at[tuple(index_at)].set(low)
    longest = extent.index(max(extent))
    index_at[longest] = (index_at[longest] + 1) % extent[longest]
    return array.at[tuple(index_at)].set(top_value)


def strengthened(entries, stream_key, source, target, parts, factor):
    def block_of(dim):
        return (jnp.arange(entries.shape[dim]) // (entries.shape[dim] // parts)).reshape((-1,) + (1,) * (entries.ndim - 1 - dim))

    one_side = jax.random.permutation(stream_key, parts)[block_of(target)]
    other_side = (block_of(target) + parts // 2) % parts
    return jnp.where((block_of(source) == one_side) | (block_of(source) == other_side), factor * entries, entries)


def level_of(rng, dims, cuts, least, high):
    loudness = 1.0
    for axis_at, parts in cuts:
        steps = jax.random.uniform(jax.random.fold_in(jax.random.fold_in(rng, 6), axis_at), (parts,), jnp.float32, least / len(cuts), high / len(cuts))
        loudness = loudness * jnp.repeat(jnp.exp(steps), dims[axis_at] // parts).reshape((-1,) + (1,) * (len(dims) - 1 - axis_at))
    return loudness


def choose_distinct(rng, rows, number_of, top, lift):
    sequence = jax.random.permutation(jax.random.fold_in(rng, 1), number_of)
    pull = sequence
    for power in range(3):
        pull = pull * pull // number_of
    pull = pull * lift // number_of
    lots = jax.random.randint(jax.random.fold_in(rng, 2), (rows, number_of), 0, 4096) + pull
    sure = jax.random.permutation(jax.random.fold_in(rng, 3), rows)[jnp.arange(number_of) % rows]
    lots = jnp.where(jnp.arange(rows)[:, None] == sure[None, :], 1 << 14, lots)
    score = lots * number_of + jnp.arange(number_of)
    return lax.top_k(score.astype(jnp.int32), top)[1].astype(jnp.int32)


def shared_out(rng, own, number, rows, number_of, top, bound, lean):
    sequence = jax.random.permutation(rng, number_of)
    crowded, common = portions_of(number_of, rows * top, bound, lean, True), portions_of(number_of, rows * top, bound, lean, False)
    places = jnp.arange(number_of)

    def named(sizes, rotation):
        used = int((sizes > 0).sum())
        fixed = max(1, used // 4)
        shifted = fixed + (places - fixed + rotation * (used - fixed)) % max(1, number_of - fixed)
        return jnp.zeros((number_of,), jnp.int32).at[sequence[jnp.where(places < fixed, places, shifted)]].set(jnp.asarray(sizes, jnp.int32))

    sizes = jnp.where(number % 4 == 0, named(crowded, number // 4), named(common, number - number // 4 - 1))
    mixed = jax.random.permutation(jax.random.fold_in(own, 3), number_of)
    donor, sink = mixed[0:number_of // 2 * 2:2], mixed[1:number_of // 2 * 2:2]
    margin = jnp.minimum(sizes[donor] - 1, bound - sizes[sink]) // 2
    margin = jnp.where((donor == sequence[0]) | (sink == sequence[0]) | (sizes[sink] == 0), 0, jnp.maximum(margin, 0))
    shifted = jax.random.randint(jax.random.fold_in(own, 4), (number_of // 2,), 0, 1 << 20) % (margin + 1)
    sizes = sizes.at[donor].add(-shifted).at[sink].add(shifted)
    items = jnp.searchsorted(jnp.cumsum(sizes), jnp.arange(rows * top), side="right").astype(jnp.int32)
    listing = items.reshape(top, rows).T
    listing = listing[jax.random.permutation(jax.random.fold_in(own, 1), rows)]
    rotation = jax.random.randint(jax.random.fold_in(own, 2), (rows, 1), 0, top)
    return jnp.take_along_axis(listing, (jnp.arange(top)[None, :] + rotation) % top, axis=1)


def portions_of(number_of, total, limit, slope, full):
    weights = [(1 << 20) // math.isqrt(standing ** slope) + 1 for standing in range(1, number_of + 1)]
    largest = limit if full else min(limit, max(-(-total // number_of), total * weights[0] // sum(weights)))
    least = 1 if total - largest >= number_of - 1 else 0
    given, spare = [largest] + [least] * (number_of - 1), total - largest - least * (number_of - 1)
    while spare > 0:
        candidates = [i for i in range(1, number_of) if given[i] < largest] or [i for i in range(1, number_of) if given[i] < limit]
        mass, left = sum([weights[i] for i in candidates]), spare
        for i in candidates:
            addition = min(limit - given[i], max(1, left * weights[i] // mass), spare)
            given[i] = given[i] + addition
            spare = spare - addition
    return np.array(given)


def noise(own_key, shape, deviation, bound, cuts=(), kind=jnp.bfloat16):
    loudness = level_of(own_key, shape, cuts, -0.22, 0.18) if cuts else 1.0
    values = jax.random.normal(own_key, shape, jnp.float32) * deviation * loudness
    return jnp.minimum(jnp.maximum(values, -bound), bound).astype(kind)


def noise_with(stream_key, dims, scale, bound, cuts, heavy, kind=jnp.bfloat16):
    values = scale * jax.random.normal(stream_key, dims, jnp.float32)
    if cuts:
        values = values * level_of(stream_key, dims, cuts, -0.22, 0.18)
    return jnp.clip(strengthened(values, jax.random.fold_in(stream_key, 3), *heavy), -bound, bound).astype(kind)


def setup_inputs(seed: int = 0) -> dict:
    key_list = jax.random.split(jax.random.key(seed), 24)
    tokens = noise(key_list[0], (STREAM_COUNT, D), 1.0, 6.0, ((0, 16), (1, 16)))
    key_cache = draw_key_cache(jax.random.fold_in(key_list[23], 71), 0)
    value_cache = noise(key_list[2], (STREAM_COUNT, HEADS, STORED_ENTRIES, HEAD_DIM), 1.0, 6.0, ((0, 16), (1, 16)))
    gate_totals = draw_gate_totals(jax.random.fold_in(key_list[23], 71), 0)
    lengths = set_ends(jax.random.randint(key_list[4], (STREAM_COUNT,), STORED_ENTRIES // 8, STORED_ENTRIES + 1), jax.random.fold_in(key_list[4], 1), STORED_ENTRIES // 8, STORED_ENTRIES).astype(jnp.int32)
    attn_gain = jnp.clip(1.0 + 0.18 * jax.random.normal(key_list[5], (D,), jnp.float32), 0.1, 1.9)
    w_query = noise(key_list[6], (D, HEADS * HEAD_DIM), D ** -0.5, 0.125, ((1, 16),))
    w_key = noise(key_list[7], (D, HEADS * HEAD_DIM), D ** -0.5, 0.125, ((1, 16),))
    w_value = noise(key_list[8], (D, HEADS * HEAD_DIM), D ** -0.5, 0.125, ((1, 16),))
    w_forget = noise(key_list[9], (D, HEADS), D ** -0.5, 0.125)
    forget_bias = jnp.clip(jax.random.uniform(key_list[10], (HEADS,), jnp.float32, -3.0, 0.0), -3.0, 0.0)
    w_attn_out = noise_with(key_list[11], (HEADS * HEAD_DIM, D), (HEADS * HEAD_DIM) ** -0.5, 0.1875, ((0, 16),), (0, 1, 16, 2.0))
    moe_gain = jnp.clip(1.0 + 0.18 * jax.random.normal(key_list[12], (D,), jnp.float32), 0.1, 1.9)
    group_ids_keys = jax.random.split(jax.random.fold_in(key_list[13], 1), STREAM_COUNT // SEQ_GRP)
    group_ids_turns = jax.random.permutation(jax.random.fold_in(key_list[13], 3), STREAM_COUNT // SEQ_GRP)
    group_ids = jax.vmap(lambda own, number: shared_out(jax.random.fold_in(key_list[13], 2), own, number, SEQ_GRP, N_EP, 1, CAP, 1))(group_ids_keys, group_ids_turns).reshape((STREAM_COUNT, 1))
    inner_ids = choose_distinct(key_list[14], STREAM_COUNT, EPG, TOPK, 0)
    group_prob = jnp.clip(0.2 + 0.8 * jax.random.uniform(key_list[15], (STREAM_COUNT,), jnp.float32) ** level_of(key_list[15], (STREAM_COUNT,), ((0, 16),), -0.2, 0.2), 0.2, 1.0)
    pair_logits = noise(key_list[16], (STREAM_COUNT, TOPK), 1.5, 6.0, ((0, 16),), jnp.float32)
    w_expert_gate = noise(key_list[17], (GROUPS, D, EPG * FFE), D ** -0.5, 0.125, ((0, 16), (2, 16)))
    w_expert_up = noise(key_list[18], (GROUPS, D, EPG * FFE), D ** -0.5, 0.125, ((0, 16), (2, 16)))
    w_expert_down = noise_with(key_list[19], (GROUPS, EPG * FFE, D), FFE ** -0.5, 0.375, ((0, 16), (1, 16)), (1, 2, 16, 2.0))
    w_dense_in = noise(key_list[20], (D, FFD), D ** -0.5, 0.125, ((1, 16),))
    w_dense_out = noise_with(key_list[21], (FFD, D), FFD ** -0.5, 0.1875, ((0, 16),), (0, 1, 16, 2.0))
    dense_gate = jnp.clip(jax.random.uniform(key_list[22], (D,), jnp.float32, -2.0, 2.0) * level_of(key_list[22], (D,), ((0, 16),), -0.4, 0.0), -2.0, 2.0)
    return {"tokens": tokens, "key_cache": key_cache, "value_cache": value_cache, "gate_totals": gate_totals, "lengths": lengths, "attn_gain": attn_gain, "w_query": w_query, "w_key": w_key, "w_value": w_value, "w_forget": w_forget, "forget_bias": forget_bias, "w_attn_out": w_attn_out, "moe_gain": moe_gain, "group_ids": group_ids, "inner_ids": inner_ids, "group_prob": group_prob, "pair_logits": pair_logits, "w_expert_gate": w_expert_gate, "w_expert_up": w_expert_up, "w_expert_down": w_expert_down, "w_dense_in": w_dense_in, "w_dense_out": w_dense_out, "dense_gate": dense_gate}


EPS = 1e-06
FLOOR = -1e+30

def norm_rows(row_data, gain_vec):
    values = row_data.astype(jnp.float32)
    factor = lax.rsqrt(lax.optimization_barrier(jnp.mean(values * values, axis=-1, keepdims=True)) + EPS)
    return (values * factor * gain_vec).astype(jnp.bfloat16)

def head_norm(values):
    factor = lax.rsqrt(lax.optimization_barrier(jnp.mean(values * values, axis=-1, keepdims=True)) + EPS)
    return (values * factor).astype(jnp.bfloat16)

def attend_one(packed):
    queries, fresh_key, fresh_value, key_rows, value_rows, totals, length, current = packed
    score_scale = HEAD_DIM ** (-0.5)
    scores = jnp.einsum('hd,hld->hl', queries.astype(jnp.float32), key_rows.astype(jnp.float32)) * score_scale
    scores = scores + current[:, None] - totals
    entry_indices = jnp.arange(STORED_ENTRIES)
    live_mask = (entry_indices < length)[None, :]
    scores = jnp.where(live_mask, scores, FLOOR)
    own_score = lax.optimization_barrier(jnp.sum(queries.astype(jnp.float32) * fresh_key.astype(jnp.float32), axis=-1)) * score_scale
    peak = jnp.maximum(lax.optimization_barrier(jnp.max(scores, axis=-1)), own_score)
    expo_terms = jnp.where(live_mask, jnp.exp(scores - peak[:, None]), 0.0)
    own_expo = jnp.exp(own_score - peak)
    denom_sum = lax.optimization_barrier(jnp.sum(expo_terms, axis=-1)) + own_expo
    weights = (expo_terms / denom_sum[:, None]).astype(jnp.bfloat16)
    own_weight = (own_expo / denom_sum).astype(jnp.bfloat16)
    attended = jnp.einsum('hl,hld->hd', weights.astype(jnp.float32), value_rows.astype(jnp.float32))
    attended = attended + own_weight.astype(jnp.float32)[:, None] * fresh_value.astype(jnp.float32)
    return attended.astype(jnp.bfloat16)

def reference(tokens, key_cache, value_cache, gate_totals, lengths, attn_gain, w_query, w_key, w_value, w_forget, forget_bias, w_attn_out, moe_gain, group_ids, inner_ids, group_prob, pair_logits, w_expert_gate, w_expert_up, w_expert_down, w_dense_in, w_dense_out, dense_gate):
    normed = norm_rows(tokens, attn_gain)
    seq_count = tokens.shape[0]

    def project(weight):
        return jnp.dot(normed, weight, preferred_element_type=jnp.float32).reshape(seq_count, HEADS, HEAD_DIM)
    queries = head_norm(project(w_query))
    new_keys = head_norm(project(w_key))
    new_values = project(w_value).astype(jnp.bfloat16)
    log_gate = jax.nn.log_sigmoid(jnp.dot(normed, w_forget, preferred_element_type=jnp.float32) + forget_bias)
    last_index = jnp.broadcast_to((lengths - 1).astype(jnp.int32)[:, None, None], (seq_count, HEADS, 1))
    last_total = jnp.take_along_axis(gate_totals, last_index, axis=2)[:, :, 0]
    new_gates = last_total + log_gate
    attended = lax.map(attend_one, (queries, new_keys, new_values, key_cache, value_cache, gate_totals, lengths, new_gates))
    projected = jnp.dot(attended.reshape(seq_count, HEADS * HEAD_DIM), w_attn_out, preferred_element_type=jnp.float32)
    residual = (tokens.astype(jnp.float32) + projected).astype(jnp.bfloat16)
    moe_in = norm_rows(residual, moe_gain)
    first_share = jax.nn.sigmoid(pair_logits[:, 0] - pair_logits[:, 1])
    pair_share = group_prob[:, None] * jnp.stack([first_share, 1.0 - first_share], axis=1)
    pair_share = lax.optimization_barrier(pair_share.astype(jnp.bfloat16)).astype(jnp.float32)
    inner_range = jnp.arange(EPG)
    spread = lax.optimization_barrier(jnp.sum(jnp.where(inner_ids[:, :, None] == inner_range[None, None, :], pair_share[:, :, None], 0.0), axis=1))

    def expert_one(packed):
        token_row, group_id, share_vec = packed
        gate_pre = jnp.dot(token_row[None, :], w_expert_gate[group_id], preferred_element_type=jnp.float32)[0]
        up_pre = jnp.dot(token_row[None, :], w_expert_up[group_id], preferred_element_type=jnp.float32)[0]
        weight_cols = jnp.repeat(share_vec, FFE)
        hidden = (jax.nn.silu(gate_pre) * up_pre * weight_cols).astype(jnp.bfloat16)
        return jnp.dot(hidden[None, :], w_expert_down[group_id], preferred_element_type=jnp.float32)[0].astype(jnp.bfloat16)
    expert_out = lax.map(expert_one, (moe_in, group_ids[:, 0], spread))
    dense_hidden = jax.nn.silu(jnp.dot(moe_in, w_dense_in, preferred_element_type=jnp.float32)).astype(jnp.bfloat16)
    dense_out = jnp.dot(dense_hidden, w_dense_out, preferred_element_type=jnp.float32)
    layer_output = residual.astype(jnp.float32) + expert_out.astype(jnp.float32) + jax.nn.sigmoid(dense_gate) * dense_out
    return (layer_output.astype(jnp.bfloat16), new_keys, new_values, new_gates)
```

```python
import jax
import jax.numpy as jnp
from jax import lax
from jax.experimental import pallas as pl
from jax.experimental.pallas import tpu as pltpu
from jax.sharding import PartitionSpec as P

EPS = 1e-06
FLOOR = -1e30
MESH = pl.DeviceIdType.MESH
N = 16
HD = 128
D = N * HD
L = 1024
FFE = 512
KB = D // 256
F32 = jnp.float32
BF = jnp.bfloat16
TP_ORDER = (8, 9, 7, 6, 10, 5, 11, 4, 12, 3, 13, 2, 14, 15, 1)
EP_ORDER = (10, 5, 15, 6, 9, 2, 8, 11, 14, 7, 13, 1, 3, 4, 12)


def iota(shape, dim):
    return lax.broadcasted_iota(jnp.int32, shape, dim)


def dot(a, b, dims=((1,), (0,))):
    return lax.dot_general(a, b, (dims, ((), ())), preferred_element_type=F32)


def rms(values):
    return lax.rsqrt(jnp.mean(values * values, axis=-1, keepdims=True) + EPS)


def sigmoid(x):
    return 1.0 / (1.0 + jnp.exp(-x))


def column_of(row):
    wide = jnp.broadcast_to(row, (N, N))
    same = iota((N, N), 0) == iota((N, N), 1)
    return jnp.sum(jnp.where(same, wide, jnp.zeros_like(wide)), axis=1, keepdims=True)


def kernel(
    tokens, key_cache, value_cache, gate_totals, lengths, attn_gain, w_query, w_key, w_value,
    w_forget, forget_bias, w_attn_out, moe_gain, group_ids, inner_ids, group_prob, pair_logits,
    w_gate, w_up, w_down, w_din, w_dout, dense_gate,
    o_layer, o_keys, o_values, o_gates,
    k_v, v_v, wqkv, wf, wo, wgu, wdn, wdi, wdo, gt_v, len_v, ag_v, fb_v, mg_v, gid_v, inn_v,
    gp_v, pl_v, tok_all, dg_all, p_v, pt_v, part2, recv2, res_all, send4, recv4, dpart,
    send5, recv5, part6, recv6, keys_v, vals_v, gates_v, lay_v,
    lsem, ssem, rsem, osem,
):
    ep = lax.axis_index("ep")
    tp = lax.axis_index("tp")
    tcol = pl.ds(pl.multiple_of(tp * HD, HD), HD)
    erow = pl.ds(pl.multiple_of(ep * N, N), N)

    barrier = pltpu.get_barrier_semaphore()
    for off in range(1, N):
        pl.semaphore_signal(
            barrier, inc=1, device_id={"tp": lax.rem(tp + off, N)}, device_id_type=MESH
        )
        pl.semaphore_signal(
            barrier, inc=1, device_id={"ep": lax.rem(ep + off, N)}, device_id_type=MESH
        )

    count = [0]

    def local(src, dst):
        copy = pltpu.make_async_copy(src, dst, lsem.at[count[0]])
        count[0] += 1
        copy.start()
        return copy

    c_tok = local(tokens, tok_all.at[:, tcol])
    c_dg = local(dense_gate, dg_all.at[:, tcol])
    c_route = [
        local(group_ids, gid_v), local(inner_ids, inn_v), local(group_prob, gp_v),
        local(pair_logits, pl_v),
    ]
    c_small = [
        local(attn_gain, ag_v), local(lengths, len_v), local(forget_bias, fb_v),
        local(gate_totals, gt_v),
    ]
    c_qkv = [
        local(w_query, wqkv.at[:, 0:HD]), local(w_key, wqkv.at[:, HD : 2 * HD]),
        local(w_value, wqkv.at[:, 2 * HD : 3 * HD]), local(w_forget, wf),
    ]
    c_k = [local(key_cache.at[s, 0], k_v.at[:, s * HD : (s + 1) * HD]) for s in range(N)]
    c_v = [local(value_cache.at[s, 0], v_v.at[:, s * HD : (s + 1) * HD]) for s in range(N)]
    c_wo = local(w_attn_out, wo)
    c_mg = local(moe_gain, mg_v)
    c_dense = [local(w_din, wdi), local(w_dout, wdo)]
    c_expert = [
        local(w_gate.at[0], wgu.at[:, 0:HD]), local(w_up.at[0], wgu.at[:, HD : 2 * HD]),
        local(w_down.at[0], wdn),
    ]

    sends = []

    def push(phase, axis, order, src_of, dst):
        me = tp if axis == "tp" else ep
        for n, off in enumerate(order):
            peer = lax.rem(me + off, N)
            copy = pltpu.make_async_remote_copy(
                src_ref=src_of(peer),
                dst_ref=dst,
                send_sem=ssem.at[phase, n],
                recv_sem=rsem.at[phase, me],
                device_id={axis: peer},
                device_id_type=MESH,
            )
            copy.start()
            sends.append(copy)

    def arrive(phase, axis, order, dst_of):
        me = tp if axis == "tp" else ep
        for n, off in reversed(list(enumerate(order))):
            peer = lax.rem(me + off, N)
            pltpu.make_async_remote_copy(
                src_ref=dst_of(peer),
                dst_ref=dst_of(peer),
                send_sem=ssem.at[phase, n],
                recv_sem=rsem.at[phase, peer],
                device_id={axis: peer},
                device_id_type=MESH,
            ).wait_recv()

    def tp_cols(ref):
        return lambda peer: ref.at[:, pl.ds(pl.multiple_of(peer * HD, HD), HD)]

    def ep_rows(ref):
        return lambda peer: ref.at[pl.ds(pl.multiple_of(peer * N, N), N), :]

    def slots(ref):
        return lambda peer: ref.at[peer]

    for copy in c_route:
        copy.wait()
    gid = gid_v[...]
    choose = (gid == iota((N, N), 1)).astype(F32)
    lower = (iota((N, N), 1) < iota((N, N), 0)).astype(F32)
    before = dot(lower.astype(BF), choose.astype(BF))
    slot_of = gid * 2 + jnp.sum(before * choose, axis=1, keepdims=True).astype(jnp.int32)
    first = sigmoid(pl_v[:, 0:1] - pl_v[:, 1:2])
    prob = column_of(gp_v[...])
    share0, share1 = prob * first, prob * (1.0 - first)
    expert = tp * HD // FFE
    inner = inn_v[...]
    spread = jnp.where(inner[:, 0:1] == expert, share0, 0.0) + jnp.where(
        inner[:, 1:2] == expert, share1, 0.0
    )
    spread = spread.astype(BF).astype(F32)
    spread_k = jnp.concatenate([spread] * KB, axis=0)
    slot_k = jnp.concatenate([slot_of] * KB, axis=0)
    rows, cols = iota((KB * N, 256), 0), iota((KB * N, 256), 1)
    pt = ((slot_k == cols // KB) & (rows // N == lax.rem(cols, KB))).astype(F32)
    pt_v[...] = pt.astype(BF)
    p_v[...] = pt.T.astype(BF)

    c_tok.wait()
    c_dg.wait()
    pl.semaphore_wait(barrier, 2 * (N - 1))
    push(0, "tp", TP_ORDER, lambda peer: tok_all.at[:, tcol], tok_all.at[:, tcol])
    push(1, "tp", TP_ORDER, lambda peer: dg_all.at[:, tcol], dg_all.at[:, tcol])

    for copy in c_small + c_qkv:
        copy.wait()
    length = column_of(len_v[...])
    arrive(0, "tp", TP_ORDER, tp_cols(tok_all))

    toks = tok_all[...].astype(F32)
    normed = (toks * rms(toks) * ag_v[...]).astype(BF)
    qkv = dot(normed, wqkv[...])
    fg = dot(normed, wf[...])
    zq, zk = qkv[:, 0:HD], qkv[:, HD : 2 * HD]
    q = (zq * rms(zq)).astype(BF)
    new_k = (zk * rms(zk)).astype(BF)
    new_v = qkv[:, 2 * HD : 3 * HD].astype(BF)
    keys_v[...] = new_k
    vals_v[...] = new_v
    o_copies = [
        pltpu.make_async_copy(keys_v, o_keys, osem.at[0]),
        pltpu.make_async_copy(vals_v, o_values, osem.at[1]),
    ]
    for copy in o_copies:
        copy.start()
    pre = fg + fb_v[...]
    pre = jnp.sum(jnp.where(iota((N, N), 1) == tp, pre, 0.0), axis=1, keepdims=True)
    log_gate = jnp.minimum(pre, 0.0) - jnp.log(1.0 + jnp.exp(-jnp.abs(pre)))
    gt = gt_v[...].reshape(N, L)
    entry = iota((N, L), 1)
    last = jnp.sum(jnp.where(entry == length - 1, gt, 0.0), axis=1, keepdims=True)
    current = last + log_gate
    gates_v[...] = current
    c_gates = pltpu.make_async_copy(gates_v, o_gates, osem.at[2])
    c_gates.start()
    o_copies.append(c_gates)

    seq = iota((N, HD), 0)
    zero = jnp.zeros_like(q)
    q_wide = jnp.concatenate([jnp.where(seq == s, q, zero) for s in range(N)], axis=1)
    for copy in c_k:
        copy.wait()
    scale = HD ** (-0.5)
    scores = jnp.concatenate(
        [dot(q_wide, k_v[c : c + 256, :], ((1,), (1,))) for c in range(0, L, 256)], axis=1
    )
    scores = scores * scale + current - gt
    live = entry < length
    scores = jnp.where(live, scores, FLOOR)
    own = jnp.sum(q.astype(F32) * new_k.astype(F32), axis=1, keepdims=True) * scale
    peak = jnp.maximum(jnp.max(scores, axis=1, keepdims=True), own)
    expo = jnp.where(live, jnp.exp(scores - peak), 0.0)
    own_expo = jnp.exp(own - peak)
    denom = jnp.sum(expo, axis=1, keepdims=True) + own_expo
    weights = (expo / denom).astype(BF)
    own_weight = (own_expo / denom).astype(BF).astype(F32)
    for copy in c_v:
        copy.wait()
    attended = own_weight * new_v.astype(F32)
    for s in range(0, N, 2):
        both = dot(weights, v_v[:, s * HD : (s + 2) * HD])
        attended += jnp.where(seq == s, both[:, 0:HD], 0.0)
        attended += jnp.where(seq == s + 1, both[:, HD : 2 * HD], 0.0)
    attended = attended.astype(BF)

    c_wo.wait()
    part2[...] = dot(attended, wo[...]).astype(BF)
    push(2, "tp", TP_ORDER, tp_cols(part2), recv2.at[tp])
    recv2[tp] = part2[:, tcol]
    own_tok = tok_all[:, tcol].astype(F32)
    arrive(2, "tp", TP_ORDER, slots(recv2))
    residual = (own_tok + jnp.sum(recv2[...].astype(F32), axis=0)).astype(BF)
    res_all[:, tcol] = residual
    push(3, "tp", TP_ORDER, lambda peer: res_all.at[:, tcol], res_all.at[:, tcol])
    c_mg.wait()
    arrive(1, "tp", TP_ORDER, tp_cols(dg_all))
    dense_scale = sigmoid(dg_all[...])
    for copy in c_dense + c_expert:
        copy.wait()
    arrive(3, "tp", TP_ORDER, tp_cols(res_all))

    res = res_all[...].astype(F32)
    moe_in = (res * rms(res) * mg_v[...]).astype(BF)
    blocks = jnp.concatenate([moe_in[:, k * 256 : (k + 1) * 256] for k in range(KB)], axis=0)
    send4[...] = dot(p_v[...], blocks).astype(BF)
    push(4, "ep", EP_ORDER, ep_rows(send4), recv4.at[erow, :])
    recv4[erow, :] = send4[erow, :]

    hidden = dot(moe_in, wdi[...])
    hidden = (hidden * sigmoid(hidden)).astype(BF)
    dense = dot(hidden, wdo[...]) * dense_scale
    for k in range(KB):
        dpart[k * N : (k + 1) * N, :] = dense[:, k * 256 : (k + 1) * 256]

    rows, cols = iota((256, 256), 0), iota((256, 256), 1)
    regroup = (lax.rem(rows, 32) * KB + rows // 32 == cols).astype(F32).astype(BF)
    ungroup = (lax.rem(cols, 32) * KB + cols // 32 == rows).astype(F32).astype(BF)
    arrive(4, "ep", EP_ORDER, ep_rows(recv4))
    xs = dot(regroup, recv4[...]).astype(BF)
    x = jnp.concatenate([xs[k * 32 : (k + 1) * 32, :] for k in range(KB)], axis=1)
    gu = dot(x, wgu[...])
    g, u = gu[:, 0:HD], gu[:, HD : 2 * HD]
    h = (g * sigmoid(g) * u).astype(BF)
    y = dot(h, wdn[...]).astype(BF)
    ys = jnp.concatenate([y[:, k * 256 : (k + 1) * 256] for k in range(KB)], axis=0)
    send5[...] = dot(ungroup, ys).astype(BF)
    push(5, "ep", EP_ORDER, ep_rows(send5), recv5.at[erow, :])
    recv5[erow, :] = send5[erow, :]
    arrive(5, "ep", EP_ORDER, ep_rows(recv5))

    total = (dot(pt_v[...], recv5[...]) * spread_k + dpart[...]).astype(BF)
    for t in range(N):
        k, half = t // 2, t % 2
        part6[t] = total[k * N : (k + 1) * N, half * HD : (half + 1) * HD]
    push(6, "tp", TP_ORDER, slots(part6), recv6.at[tp])
    recv6[tp] = part6[tp]
    own_res = res_all[:, tcol].astype(F32)
    arrive(6, "tp", TP_ORDER, slots(recv6))
    lay_v[...] = (own_res + jnp.sum(recv6[...].astype(F32), axis=0)).astype(BF)
    c_lay = pltpu.make_async_copy(lay_v, o_layer, osem.at[3])
    c_lay.start()
    o_copies.append(c_lay)
    for copy in sends:
        copy.wait_send()
    for copy in o_copies:
        copy.wait()


def body(
    tokens, key_cache, value_cache, gate_totals, lengths, attn_gain, w_query, w_key, w_value,
    w_forget, forget_bias, w_attn_out, moe_gain, group_ids, inner_ids, group_prob, pair_logits,
    w_expert_gate, w_expert_up, w_expert_down, w_dense_in, w_dense_out, dense_gate,
):
    any_space = pl.BlockSpec(memory_space=pl.ANY)
    vmem = pltpu.VMEM
    outs = pl.pallas_call(
        kernel,
        out_shape=(
            jax.ShapeDtypeStruct((N, HD), BF),
            jax.ShapeDtypeStruct((N, HD), BF),
            jax.ShapeDtypeStruct((N, HD), BF),
            jax.ShapeDtypeStruct((N, 1), F32),
        ),
        in_specs=[any_space] * 23,
        out_specs=[any_space] * 4,
        scratch_shapes=[
            vmem((L, D), BF), vmem((L, D), BF), vmem((D, 3 * HD), BF), vmem((D, N), BF),
            vmem((HD, D), BF), vmem((D, 2 * HD), BF), vmem((HD, D), BF), vmem((D, HD), BF),
            vmem((HD, D), BF), vmem((N, 1, L), F32), vmem((1, N), jnp.int32), vmem((1, D), F32),
            vmem((1, N), F32), vmem((1, D), F32), vmem((N, 1), jnp.int32),
            vmem((N, 2), jnp.int32), vmem((1, N), F32), vmem((N, 2), F32),
            vmem((N, D), BF), vmem((1, D), F32), vmem((256, KB * N), BF), vmem((KB * N, 256), BF),
            vmem((N, D), BF), vmem((N, N, HD), BF), vmem((N, D), BF), vmem((256, 256), BF),
            vmem((256, 256), BF), vmem((KB * N, 256), F32), vmem((256, 256), BF),
            vmem((256, 256), BF), vmem((N, N, HD), BF), vmem((N, N, HD), BF),
            vmem((N, HD), BF), vmem((N, HD), BF), vmem((N, 1), F32), vmem((N, HD), BF),
            pltpu.SemaphoreType.DMA((64,)), pltpu.SemaphoreType.DMA((7, N)),
            pltpu.SemaphoreType.DMA((7, N)), pltpu.SemaphoreType.DMA((4,)),
        ],
        compiler_params=pltpu.CompilerParams(
            collective_id=0, has_side_effects=True, vmem_limit_bytes=48 * 1024 * 1024
        ),
    )(
        tokens, key_cache, value_cache, gate_totals, lengths.reshape(1, N),
        attn_gain.reshape(1, D), w_query, w_key, w_value, w_forget, forget_bias.reshape(1, N),
        w_attn_out, moe_gain.reshape(1, D), group_ids, inner_ids, group_prob.reshape(1, N),
        pair_logits, w_expert_gate, w_expert_up, w_expert_down, w_dense_in, w_dense_out,
        dense_gate.reshape(1, HD),
    )
    layer, keys, values, gates = outs
    return (layer, keys.reshape(N, 1, HD), values.reshape(N, 1, HD), gates)


def solution(mesh):
    placed = (
        P("ep", "tp"),
        P("ep", "tp", None, None),
        P("ep", "tp", None, None),
        P("ep", "tp", None),
        P("ep"),
        P(),
        P(None, "tp"),
        P(None, "tp"),
        P(None, "tp"),
        P(),
        P(),
        P("tp", None),
        P(),
        P("ep", None),
        P("ep", None),
        P("ep"),
        P("ep", None),
        P("ep", None, "tp"),
        P("ep", None, "tp"),
        P("ep", "tp", None),
        P(None, "tp"),
        P("tp", None),
        P("tp"),
    )
    return jax.shard_map(
        body,
        mesh=mesh,
        in_specs=placed,
        out_specs=(P("ep", "tp"), P("ep", "tp", None), P("ep", "tp", None), P("ep", "tp")),
        check_vma=False,
    )
```

```python
import jax
import jax.numpy as jnp
from jax import lax
from jax.experimental import pallas as pl
from jax.experimental.pallas import tpu as pltpu
from jax.sharding import PartitionSpec as P

EPS = 1e-06
FLOOR = -1e30
MESH = pl.DeviceIdType.MESH
N = 16
HD = 128
D = N * HD
L = 1024
FFE = 512
KB = D // 256
F32 = jnp.float32
BF = jnp.bfloat16
TP_ORDER = (8, 9, 7, 6, 10, 5, 11, 4, 12, 3, 13, 2, 14, 15, 1)
EP_ORDER = (10, 5, 15, 6, 9, 2, 8, 11, 14, 7, 13, 1, 3, 4, 12)


def iota(shape, dim):
    return lax.broadcasted_iota(jnp.int32, shape, dim)


def dot(a, b, dims=((1,), (0,))):
    return lax.dot_general(a, b, (dims, ((), ())), preferred_element_type=F32)


def rms(values):
    return lax.rsqrt(jnp.mean(values * values, axis=-1, keepdims=True) + EPS)


def sigmoid(x):
    return 1.0 / (1.0 + jnp.exp(-x))


def column_of(row):
    wide = jnp.broadcast_to(row, (N, N))
    same = iota((N, N), 0) == iota((N, N), 1)
    return jnp.sum(jnp.where(same, wide, jnp.zeros_like(wide)), axis=1, keepdims=True)


def kernel(
    tokens, key_cache, value_cache, gate_totals, lengths, attn_gain, w_query, w_key, w_value,
    w_forget, forget_bias, w_attn_out, moe_gain, group_ids, inner_ids, group_prob, pair_logits,
    w_gate, w_up, w_down, w_din, w_dout, dense_gate,
    o_layer, o_keys, o_values, o_gates,
    k_v, v_v, wqkv, wf, wo, wgu, wdn, wdi, wdo, gt_v, len_v, ag_v, fb_v, mg_v, gid_v, inn_v,
    gp_v, pl_v, tok_all, dg_all, p_v, pt_v, part2, recv2, res_all, send4, recv4, dpart,
    send5, recv5, part6, recv6, keys_v, vals_v, gates_v, lay_v,
    lsem, ssem, rsem, osem,
):
    ep = lax.axis_index("ep")
    tp = lax.axis_index("tp")
    tcol = pl.ds(pl.multiple_of(tp * HD, HD), HD)
    erow = pl.ds(pl.multiple_of(ep * N, N), N)

    barrier = pltpu.get_barrier_semaphore()
    for off in range(1, N):
        pl.semaphore_signal(
            barrier, inc=1, device_id={"tp": lax.rem(tp + off, N)}, device_id_type=MESH
        )
        pl.semaphore_signal(
            barrier, inc=1, device_id={"ep": lax.rem(ep + off, N)}, device_id_type=MESH
        )

    count = [0]

    def local(src, dst):
        copy = pltpu.make_async_copy(src, dst, lsem.at[count[0]])
        count[0] += 1
        copy.start()
        return copy

    c_tok = local(tokens, tok_all.at[:, tcol])
    c_dg = local(dense_gate, dg_all.at[:, tcol])
    c_route = [
        local(group_ids, gid_v), local(inner_ids, inn_v), local(group_prob, gp_v),
        local(pair_logits, pl_v),
    ]
    c_small = [
        local(attn_gain, ag_v), local(lengths, len_v), local(forget_bias, fb_v),
        local(gate_totals, gt_v),
    ]
    c_qkv = [
        local(w_query, wqkv.at[:, 0:HD]), local(w_key, wqkv.at[:, HD : 2 * HD]),
        local(w_value, wqkv.at[:, 2 * HD : 3 * HD]), local(w_forget, wf),
    ]
    c_k = [local(key_cache.at[s, 0], k_v.at[:, s * HD : (s + 1) * HD]) for s in range(N)]
    c_v = [local(value_cache.at[s, 0], v_v.at[:, s * HD : (s + 1) * HD]) for s in range(N)]
    c_wo = local(w_attn_out, wo)
    c_mg = local(moe_gain, mg_v)
    c_dense = [local(w_din, wdi), local(w_dout, wdo)]
    c_expert = [
        local(w_gate.at[0], wgu.at[:, 0:HD]), local(w_up.at[0], wgu.at[:, HD : 2 * HD]),
        local(w_down.at[0], wdn),
    ]

    sends = []

    def push(phase, axis, order, src_of, dst):
        me = tp if axis == "tp" else ep
        for n, off in enumerate(order):
            peer = lax.rem(me + off, N)
            copy = pltpu.make_async_remote_copy(
                src_ref=src_of(peer),
                dst_ref=dst,
                send_sem=ssem.at[phase, n],
                recv_sem=rsem.at[phase, me],
                device_id={axis: peer},
                device_id_type=MESH,
            )
            copy.start()
            sends.append(copy)

    def arrive(phase, axis, order, dst_of):
        me = tp if axis == "tp" else ep
        for n, off in reversed(list(enumerate(order))):
            peer = lax.rem(me + off, N)
            pltpu.make_async_remote_copy(
                src_ref=dst_of(peer),
                dst_ref=dst_of(peer),
                send_sem=ssem.at[phase, n],
                recv_sem=rsem.at[phase, peer],
                device_id={axis: peer},
                device_id_type=MESH,
            ).wait_recv()

    def tp_cols(ref):
        return lambda peer: ref.at[:, pl.ds(pl.multiple_of(peer * HD, HD), HD)]

    def ep_rows(ref):
        return lambda peer: ref.at[pl.ds(pl.multiple_of(peer * N, N), N), :]

    def slots(ref):
        return lambda peer: ref.at[peer]

    for copy in c_route:
        copy.wait()
    gid = column_of(gid_v[...])
    choose = (gid == iota((N, N), 1)).astype(F32)
    lower = (iota((N, N), 1) < iota((N, N), 0)).astype(F32)
    before = dot(lower.astype(BF), choose.astype(BF))
    slot_of = gid * 2 + jnp.sum(before * choose, axis=1, keepdims=True).astype(jnp.int32)
    first = sigmoid(pl_v[0:1, :] - pl_v[1:2, :])
    share0, share1 = gp_v[...] * first, gp_v[...] * (1.0 - first)
    expert = tp * HD // FFE
    inner = inn_v[...]
    spread = jnp.where(inner[0:1, :] == expert, share0, 0.0) + jnp.where(
        inner[1:2, :] == expert, share1, 0.0
    )
    spread = column_of(spread.astype(BF).astype(F32))
    spread_k = jnp.concatenate([spread] * KB, axis=0)
    slot_k = jnp.concatenate([slot_of] * KB, axis=0)
    rows, cols = iota((KB * N, 256), 0), iota((KB * N, 256), 1)
    pt = ((slot_k == cols // KB) & (rows // N == lax.rem(cols, KB))).astype(F32)
    pt_v[...] = pt.astype(BF)
    p_v[...] = pt.T.astype(BF)

    c_tok.wait()
    c_dg.wait()
    pl.semaphore_wait(barrier, 2 * (N - 1))
    push(0, "tp", TP_ORDER, lambda peer: tok_all.at[:, tcol], tok_all.at[:, tcol])
    push(1, "tp", TP_ORDER, lambda peer: dg_all.at[:, tcol], dg_all.at[:, tcol])

    for copy in c_small + c_qkv:
        copy.wait()
    length = column_of(len_v[...])
    arrive(0, "tp", TP_ORDER, tp_cols(tok_all))

    toks = tok_all[...].astype(F32)
    normed = (toks * rms(toks) * ag_v[...]).astype(BF)
    qkv = dot(normed, wqkv[...])
    fg = dot(normed, wf[...], ((1,), (1,)))
    zq, zk = qkv[:, 0:HD], qkv[:, HD : 2 * HD]
    q = (zq * rms(zq)).astype(BF)
    new_k = (zk * rms(zk)).astype(BF)
    new_v = qkv[:, 2 * HD : 3 * HD].astype(BF)
    keys_v[...] = new_k
    vals_v[...] = new_v
    o_copies = [
        pltpu.make_async_copy(keys_v, o_keys, osem.at[0]),
        pltpu.make_async_copy(vals_v, o_values, osem.at[1]),
    ]
    for copy in o_copies:
        copy.start()
    pre = fg + fb_v[...]
    pre = jnp.sum(jnp.where(iota((N, N), 1) == tp, pre, 0.0), axis=1, keepdims=True)
    log_gate = jnp.minimum(pre, 0.0) - jnp.log(1.0 + jnp.exp(-jnp.abs(pre)))
    gt = gt_v[...].reshape(N, L)
    entry = iota((N, L), 1)
    last = jnp.sum(jnp.where(entry == length - 1, gt, 0.0), axis=1, keepdims=True)
    current = last + log_gate
    same = iota((N, N), 0) == iota((N, N), 1)
    gates_v[...] = jnp.sum(jnp.where(same, jnp.broadcast_to(current, (N, N)), 0.0), axis=0, keepdims=True)
    c_gates = pltpu.make_async_copy(gates_v, o_gates, osem.at[2])
    c_gates.start()
    o_copies.append(c_gates)

    seq = iota((N, HD), 0)
    zero = jnp.zeros_like(q)
    q_wide = jnp.concatenate([jnp.where(seq == s, q, zero) for s in range(N)], axis=1)
    for copy in c_k:
        copy.wait()
    scale = HD ** (-0.5)
    scores = jnp.concatenate(
        [dot(q_wide, k_v[c : c + 256, :], ((1,), (1,))) for c in range(0, L, 256)], axis=1
    )
    scores = scores * scale + current - gt
    live = entry < length
    scores = jnp.where(live, scores, FLOOR)
    own = jnp.sum(q.astype(F32) * new_k.astype(F32), axis=1, keepdims=True) * scale
    peak = jnp.maximum(jnp.max(scores, axis=1, keepdims=True), own)
    expo = jnp.where(live, jnp.exp(scores - peak), 0.0)
    own_expo = jnp.exp(own - peak)
    denom = jnp.sum(expo, axis=1, keepdims=True) + own_expo
    weights = (expo / denom).astype(BF)
    own_weight = (own_expo / denom).astype(BF).astype(F32)
    for copy in c_v:
        copy.wait()
    attended = own_weight * new_v.astype(F32)
    for s in range(0, N, 2):
        both = dot(weights, v_v[:, s * HD : (s + 2) * HD])
        attended += jnp.where(seq == s, both[:, 0:HD], 0.0)
        attended += jnp.where(seq == s + 1, both[:, HD : 2 * HD], 0.0)
    attended = attended.astype(BF)

    c_wo.wait()
    part2[...] = dot(attended, wo[...]).astype(BF)
    push(2, "tp", TP_ORDER, tp_cols(part2), recv2.at[tp])
    recv2[tp] = part2[:, tcol]
    own_tok = tok_all[:, tcol].astype(F32)
    arrive(2, "tp", TP_ORDER, slots(recv2))
    residual = (own_tok + jnp.sum(recv2[...].astype(F32), axis=0)).astype(BF)
    res_all[:, tcol] = residual
    push(3, "tp", TP_ORDER, lambda peer: res_all.at[:, tcol], res_all.at[:, tcol])
    c_mg.wait()
    arrive(1, "tp", TP_ORDER, tp_cols(dg_all))
    dense_scale = sigmoid(dg_all[...])
    for copy in c_dense + c_expert:
        copy.wait()
    arrive(3, "tp", TP_ORDER, tp_cols(res_all))

    res = res_all[...].astype(F32)
    moe_in = (res * rms(res) * mg_v[...]).astype(BF)
    blocks = jnp.concatenate([moe_in[:, k * 256 : (k + 1) * 256] for k in range(KB)], axis=0)
    send4[...] = dot(p_v[...], blocks).astype(BF)
    push(4, "ep", EP_ORDER, ep_rows(send4), recv4.at[erow, :])
    recv4[erow, :] = send4[erow, :]

    hidden = dot(moe_in, wdi[...])
    hidden = (hidden * sigmoid(hidden)).astype(BF)
    dense = dot(hidden, wdo[...]) * dense_scale
    for k in range(KB):
        dpart[k * N : (k + 1) * N, :] = dense[:, k * 256 : (k + 1) * 256]

    rows, cols = iota((256, 256), 0), iota((256, 256), 1)
    regroup = (lax.rem(rows, 32) * KB + rows // 32 == cols).astype(F32).astype(BF)
    ungroup = (lax.rem(cols, 32) * KB + cols // 32 == rows).astype(F32).astype(BF)
    arrive(4, "ep", EP_ORDER, ep_rows(recv4))
    xs = dot(regroup, recv4[...]).astype(BF)
    x = jnp.concatenate([xs[k * 32 : (k + 1) * 32, :] for k in range(KB)], axis=1)
    gu = dot(x, wgu[...])
    g, u = gu[:, 0:HD], gu[:, HD : 2 * HD]
    h = (g * sigmoid(g) * u).astype(BF)
    y = dot(h, wdn[...]).astype(BF)
    ys = jnp.concatenate([y[:, k * 256 : (k + 1) * 256] for k in range(KB)], axis=0)
    send5[...] = dot(ungroup, ys).astype(BF)
    push(5, "ep", EP_ORDER, ep_rows(send5), recv5.at[erow, :])
    recv5[erow, :] = send5[erow, :]
    arrive(5, "ep", EP_ORDER, ep_rows(recv5))

    total = (dot(pt_v[...], recv5[...]) * spread_k + dpart[...]).astype(BF)
    for t in range(N):
        k, half = t // 2, t % 2
        part6[t] = total[k * N : (k + 1) * N, half * HD : (half + 1) * HD]
    push(6, "tp", TP_ORDER, slots(part6), recv6.at[tp])
    recv6[tp] = part6[tp]
    own_res = res_all[:, tcol].astype(F32)
    arrive(6, "tp", TP_ORDER, slots(recv6))
    lay_v[...] = (own_res + jnp.sum(recv6[...].astype(F32), axis=0)).astype(BF)
    c_lay = pltpu.make_async_copy(lay_v, o_layer, osem.at[3])
    c_lay.start()
    o_copies.append(c_lay)
    for copy in sends:
        copy.wait_send()
    for copy in o_copies:
        copy.wait()


def body(
    tokens, key_cache, value_cache, gate_totals, lengths, attn_gain, w_query, w_key, w_value,
    w_forget, forget_bias, w_attn_out, moe_gain, group_ids, inner_ids, group_prob, pair_logits,
    w_expert_gate, w_expert_up, w_expert_down, w_dense_in, w_dense_out, dense_gate,
):
    any_space = pl.BlockSpec(memory_space=pl.ANY)
    vmem = pltpu.VMEM
    outs = pl.pallas_call(
        kernel,
        out_shape=(
            jax.ShapeDtypeStruct((N, HD), BF),
            jax.ShapeDtypeStruct((N, HD), BF),
            jax.ShapeDtypeStruct((N, HD), BF),
            jax.ShapeDtypeStruct((1, N), F32),
        ),
        in_specs=[any_space] * 23,
        out_specs=[any_space] * 4,
        scratch_shapes=[
            vmem((L, D), BF), vmem((L, D), BF), vmem((D, 3 * HD), BF), vmem((N, D), BF),
            vmem((HD, D), BF), vmem((D, 2 * HD), BF), vmem((HD, D), BF), vmem((D, HD), BF),
            vmem((HD, D), BF), vmem((N, 1, L), F32), vmem((1, N), jnp.int32), vmem((1, D), F32),
            vmem((1, N), F32), vmem((1, D), F32), vmem((1, N), jnp.int32),
            vmem((2, N), jnp.int32), vmem((1, N), F32), vmem((2, N), F32),
            vmem((N, D), BF), vmem((1, D), F32), vmem((256, KB * N), BF), vmem((KB * N, 256), BF),
            vmem((N, D), BF), vmem((N, N, HD), BF), vmem((N, D), BF), vmem((256, 256), BF),
            vmem((256, 256), BF), vmem((KB * N, 256), F32), vmem((256, 256), BF),
            vmem((256, 256), BF), vmem((N, N, HD), BF), vmem((N, N, HD), BF),
            vmem((N, HD), BF), vmem((N, HD), BF), vmem((1, N), F32), vmem((N, HD), BF),
            pltpu.SemaphoreType.DMA((64,)), pltpu.SemaphoreType.DMA((7, N)),
            pltpu.SemaphoreType.DMA((7, N)), pltpu.SemaphoreType.DMA((4,)),
        ],
        compiler_params=pltpu.CompilerParams(
            collective_id=0, has_side_effects=True, vmem_limit_bytes=67_043_328
        ),
    )(
        tokens, key_cache, value_cache, gate_totals, lengths.reshape(1, N),
        attn_gain.reshape(1, D), w_query, w_key, w_value, w_forget.T, forget_bias.reshape(1, N),
        w_attn_out, moe_gain.reshape(1, D), group_ids.T, inner_ids.T,
        group_prob.reshape(1, N), pair_logits.T, w_expert_gate, w_expert_up, w_expert_down, w_dense_in, w_dense_out,
        dense_gate.reshape(1, HD),
    )
    layer, keys, values, gates = outs
    return (layer, keys.reshape(N, 1, HD), values.reshape(N, 1, HD), gates.reshape(N, 1))


def solution(mesh):
    placed = (
        P("ep", "tp"),
        P("ep", "tp", None, None),
        P("ep", "tp", None, None),
        P("ep", "tp", None),
        P("ep"),
        P(),
        P(None, "tp"),
        P(None, "tp"),
        P(None, "tp"),
        P(),
        P(),
        P("tp", None),
        P(),
        P("ep", None),
        P("ep", None),
        P("ep"),
        P("ep", None),
        P("ep", None, "tp"),
        P("ep", None, "tp"),
        P("ep", "tp", None),
        P(None, "tp"),
        P("tp", None),
        P("tp"),
    )
    return jax.shard_map(
        body,
        mesh=mesh,
        in_specs=placed,
        out_specs=(P("ep", "tp"), P("ep", "tp", None), P("ep", "tp", None), P("ep", "tp")),
        check_vma=False,
    )
```

```python
import jax
import jax.numpy as jnp
from jax import lax
from jax.experimental import pallas as pl
from jax.experimental.pallas import tpu as pltpu
from jax.sharding import PartitionSpec as P

EPS = 1e-06
FLOOR = -1e30
MESH = pl.DeviceIdType.MESH
N = 16
HD = 128
D = N * HD
L = 1024
FFE = 512
F32 = jnp.float32
BF = jnp.bfloat16
TP_ORDER = (8, 9, 7, 6, 10, 5, 11, 4, 12, 3, 13, 2, 14, 15, 1)
EP_ORDER = (10, 5, 15, 6, 9, 2, 8, 11, 14, 7, 13, 1, 3, 4, 12)


def iota(shape, dim):
    return lax.broadcasted_iota(jnp.int32, shape, dim)


def dot(a, b, dims=((1,), (0,))):
    return lax.dot_general(a, b, (dims, ((), ())), preferred_element_type=F32)


def rms(values):
    return lax.rsqrt(jnp.mean(values * values, axis=-1, keepdims=True) + EPS)


def sigmoid(x):
    return 1.0 / (1.0 + jnp.exp(-x))


def column_of(row):
    wide = jnp.broadcast_to(row, (N, N))
    same = iota((N, N), 0) == iota((N, N), 1)
    return jnp.sum(jnp.where(same, wide, jnp.zeros_like(wide)), axis=1, keepdims=True)


def kernel(
    tokens, key_cache, value_cache, gate_totals, lengths, attn_gain, w_query, w_key, w_value,
    w_forget, forget_bias, w_attn_out, moe_gain, group_ids, inner_ids, group_prob, pair_logits,
    w_gate, w_up, w_down, w_din, w_dout, dense_gate,
    o_layer, o_keys, o_values, o_gates,
    k_v, v_v, wqkv, wf, wo, wgu, wdn, wdi, wdo, gt_v, len_v, ag_v, fb_v, mg_v, gid_v, inn_v,
    gp_v, pl_v, tok_all, dg_all, part2, recv2, res_all, send4, recv4, dpart,
    send5, recv5, part6, recv6, keys_v, vals_v, gates_v, lay_v,
    lsem, ssem, rsem, osem,
):
    ep = lax.axis_index("ep")
    tp = lax.axis_index("tp")
    tcol = pl.ds(pl.multiple_of(tp * HD, HD), HD)
    erow = pl.ds(pl.multiple_of(ep * 2, 2), 2)

    count = [0]

    def local(src, dst):
        copy = pltpu.make_async_copy(src, dst, lsem.at[count[0]])
        count[0] += 1
        copy.start()
        return copy

    c_tok = local(tokens, tok_all.at[:, tcol])
    c_dg = local(dense_gate, dg_all.at[:, tcol])
    barrier = pltpu.get_barrier_semaphore()
    for off in range(1, N):
        pl.semaphore_signal(
            barrier, inc=1, device_id={"tp": lax.rem(tp + off, N)}, device_id_type=MESH
        )
        pl.semaphore_signal(
            barrier, inc=1, device_id={"ep": lax.rem(ep + off, N)}, device_id_type=MESH
        )
    c_route = [
        local(group_ids, gid_v), local(inner_ids, inn_v), local(group_prob, gp_v),
        local(pair_logits, pl_v),
    ]
    c_small = [
        local(attn_gain, ag_v), local(lengths, len_v), local(forget_bias, fb_v),
        local(gate_totals, gt_v),
    ]
    c_qkv = [
        local(w_query, wqkv.at[:, 0:HD]), local(w_key, wqkv.at[:, HD : 2 * HD]),
        local(w_value, wqkv.at[:, 2 * HD : 3 * HD]), local(w_forget, wf),
    ]
    c_k = [local(key_cache.at[s, 0], k_v.at[:, s * HD : (s + 1) * HD]) for s in range(N)]
    c_v = [local(value_cache.at[s, 0], v_v.at[:, s * HD : (s + 1) * HD]) for s in range(N)]
    c_wo = local(w_attn_out, wo)
    c_mg = local(moe_gain, mg_v)
    c_dense = [local(w_din, wdi), local(w_dout, wdo)]
    c_expert = [
        local(w_gate.at[0], wgu.at[:, 0:HD]), local(w_up.at[0], wgu.at[:, HD : 2 * HD]),
        local(w_down.at[0], wdn),
    ]

    sends = []

    def push(phase, axis, order, src_of, dst):
        me = tp if axis == "tp" else ep
        for n, off in enumerate(order):
            peer = lax.rem(me + off, N)
            copy = pltpu.make_async_remote_copy(
                src_ref=src_of(peer),
                dst_ref=dst,
                send_sem=ssem.at[phase, n],
                recv_sem=rsem.at[phase, me],
                device_id={axis: peer},
                device_id_type=MESH,
            )
            copy.start()
            sends.append(copy)

    def arrive(phase, axis, order, dst_of):
        me = tp if axis == "tp" else ep
        for n, off in reversed(list(enumerate(order))):
            peer = lax.rem(me + off, N)
            pltpu.make_async_remote_copy(
                src_ref=dst_of(peer),
                dst_ref=dst_of(peer),
                send_sem=ssem.at[phase, n],
                recv_sem=rsem.at[phase, peer],
                device_id={axis: peer},
                device_id_type=MESH,
            ).wait_recv()

    def tp_cols(ref):
        return lambda peer: ref.at[:, pl.ds(pl.multiple_of(peer * HD, HD), HD)]

    def ep_rows(ref):
        return lambda peer: ref.at[pl.ds(pl.multiple_of(peer * 2, 2), 2), :]

    def slots(ref):
        return lambda peer: ref.at[peer]

    c_tok.wait()
    pl.semaphore_wait(barrier, 2 * (N - 1))
    push(0, "tp", TP_ORDER, lambda peer: tok_all.at[:, tcol], tok_all.at[:, tcol])
    c_dg.wait()
    push(1, "tp", TP_ORDER, lambda peer: dg_all.at[:, tcol], dg_all.at[:, tcol])

    for copy in c_route:
        copy.wait()
    gid = gid_v[...]
    gid_col = column_of(gid)
    same = gid_col == jnp.broadcast_to(gid, (N, N))
    earlier = iota((N, N), 0) < iota((N, N), 1)
    rank = jnp.sum((same & earlier).astype(jnp.int32), axis=0, keepdims=True)
    later = iota((N, N), 1) < iota((N, N), 0)
    rank_col = jnp.sum((same & later).astype(jnp.int32), axis=1, keepdims=True)
    send_map = (gid * 2 + rank == iota((2 * N, N), 0)).astype(F32).astype(BF)
    back_map = (gid_col * 2 + rank_col == iota((N, 2 * N), 1)).astype(F32).astype(BF)
    first = sigmoid(pl_v[0:1, :] - pl_v[1:2, :])
    share0, share1 = gp_v[...] * first, gp_v[...] * (1.0 - first)
    expert = tp * HD // FFE
    inner = inn_v[...]
    spread = jnp.where(inner[0:1, :] == expert, share0, 0.0) + jnp.where(
        inner[1:2, :] == expert, share1, 0.0
    )
    spread = column_of(spread.astype(BF).astype(F32))
    for copy in c_small + c_qkv:
        copy.wait()
    length = column_of(len_v[...])
    gt = gt_v[...].reshape(N, L)
    entry = iota((N, L), 1)
    live = entry < length
    last = jnp.sum(jnp.where(entry == length - 1, gt, 0.0), axis=1, keepdims=True)
    arrive(0, "tp", TP_ORDER, tp_cols(tok_all))

    toks = tok_all[...].astype(F32)
    normed = (toks * rms(toks) * ag_v[...]).astype(BF)
    qkv = dot(normed, wqkv[...])
    fg = dot(normed, wf[...], ((1,), (1,)))
    zq, zk = qkv[:, 0:HD], qkv[:, HD : 2 * HD]
    q = (zq * rms(zq)).astype(BF)
    new_k = (zk * rms(zk)).astype(BF)
    new_v = qkv[:, 2 * HD : 3 * HD].astype(BF)
    keys_v[...] = new_k
    vals_v[...] = new_v
    o_copies = [
        pltpu.make_async_copy(keys_v, o_keys, osem.at[0]),
        pltpu.make_async_copy(vals_v, o_values, osem.at[1]),
    ]
    for copy in o_copies:
        copy.start()
    pre = fg + fb_v[...]
    pre = jnp.sum(jnp.where(iota((N, N), 1) == tp, pre, 0.0), axis=1, keepdims=True)
    log_gate = jnp.minimum(pre, 0.0) - jnp.log(1.0 + jnp.exp(-jnp.abs(pre)))
    current = last + log_gate
    same = iota((N, N), 0) == iota((N, N), 1)
    gates_v[...] = jnp.sum(jnp.where(same, jnp.broadcast_to(current, (N, N)), 0.0), axis=0, keepdims=True)
    c_gates = pltpu.make_async_copy(gates_v, o_gates, osem.at[2])
    c_gates.start()
    o_copies.append(c_gates)

    seq = iota((N, HD), 0)
    zero = jnp.zeros_like(q)
    q_wide = jnp.concatenate([jnp.where(seq == s, q, zero) for s in range(N)], axis=1)
    for copy in c_k:
        copy.wait()
    scale = HD ** (-0.5)
    scores = jnp.concatenate(
        [dot(q_wide, k_v[c : c + 256, :], ((1,), (1,))) for c in range(0, L, 256)], axis=1
    )
    scores = scores * scale + current - gt
    scores = jnp.where(live, scores, FLOOR)
    own = jnp.sum(q.astype(F32) * new_k.astype(F32), axis=1, keepdims=True) * scale
    peak = jnp.maximum(jnp.max(scores, axis=1, keepdims=True), own)
    expo = jnp.where(live, jnp.exp(scores - peak), 0.0)
    own_expo = jnp.exp(own - peak)
    denom = jnp.sum(expo, axis=1, keepdims=True) + own_expo
    weights = (expo / denom).astype(BF)
    own_weight = (own_expo / denom).astype(BF).astype(F32)
    for copy in c_v:
        copy.wait()
    attended = own_weight * new_v.astype(F32)
    for s in range(0, N, 2):
        both = dot(weights, v_v[:, s * HD : (s + 2) * HD])
        attended += jnp.where(seq == s, both[:, 0:HD], 0.0)
        attended += jnp.where(seq == s + 1, both[:, HD : 2 * HD], 0.0)
    attended = attended.astype(BF)

    c_wo.wait()
    part2[...] = dot(attended, wo[...]).astype(BF)
    push(2, "tp", TP_ORDER, tp_cols(part2), recv2.at[tp])
    recv2[tp] = part2[:, tcol]
    own_tok = tok_all[:, tcol].astype(F32)
    arrive(2, "tp", TP_ORDER, slots(recv2))
    residual = (own_tok + jnp.sum(recv2[...].astype(F32), axis=0)).astype(BF)
    res_all[:, tcol] = residual
    push(3, "tp", TP_ORDER, lambda peer: res_all.at[:, tcol], res_all.at[:, tcol])
    c_mg.wait()
    arrive(1, "tp", TP_ORDER, tp_cols(dg_all))
    dense_scale = sigmoid(dg_all[...])
    for copy in c_dense + c_expert:
        copy.wait()
    arrive(3, "tp", TP_ORDER, tp_cols(res_all))

    res = res_all[...].astype(F32)
    moe_in = (res * rms(res) * mg_v[...]).astype(BF)
    send4[...] = dot(send_map, moe_in).astype(BF)
    push(4, "ep", EP_ORDER, ep_rows(send4), recv4.at[erow, :])

    hidden = dot(moe_in, wdi[...])
    hidden = (hidden * sigmoid(hidden)).astype(BF)
    dpart[...] = dot(hidden, wdo[...]) * dense_scale

    arrive(4, "ep", EP_ORDER, ep_rows(recv4))
    mine = iota((2 * N, D), 0) // 2 == ep
    x = jnp.where(mine, send4[...], recv4[...])
    gu = dot(x, wgu[...])
    g, u = gu[:, 0:HD], gu[:, HD : 2 * HD]
    h = (g * sigmoid(g) * u).astype(BF)
    send5[...] = dot(h, wdn[...]).astype(BF)
    push(5, "ep", EP_ORDER, ep_rows(send5), recv5.at[erow, :])
    arrive(5, "ep", EP_ORDER, ep_rows(recv5))

    part6[...] = (dot(back_map, jnp.where(mine, send5[...], recv5[...])) * spread + dpart[...]).astype(BF)
    push(6, "tp", TP_ORDER, tp_cols(part6), recv6.at[tp])
    recv6[tp] = part6[:, tcol]
    own_res = res_all[:, tcol].astype(F32)
    arrive(6, "tp", TP_ORDER, slots(recv6))
    lay_v[...] = (own_res + jnp.sum(recv6[...].astype(F32), axis=0)).astype(BF)
    c_lay = pltpu.make_async_copy(lay_v, o_layer, osem.at[3])
    c_lay.start()
    o_copies.append(c_lay)
    for copy in sends:
        copy.wait_send()
    for copy in o_copies:
        copy.wait()


def writer(*refs):
    ins, outs, held, sem = refs[0:4], refs[4:8], refs[8:12], refs[12]
    reads = [pltpu.make_async_copy(ins[i], held[i], sem.at[0, i]) for i in range(4)]
    writes = [pltpu.make_async_copy(held[i], outs[i], sem.at[1, i]) for i in range(4)]
    for copy in reads:
        copy.start()
    for read, write in zip(reads, writes):
        read.wait()
        write.start()
    for copy in writes:
        copy.wait()


def body(
    tokens, key_cache, value_cache, gate_totals, lengths, attn_gain, w_query, w_key, w_value,
    w_forget, forget_bias, w_attn_out, moe_gain, group_ids, inner_ids, group_prob, pair_logits,
    w_expert_gate, w_expert_up, w_expert_down, w_dense_in, w_dense_out, dense_gate,
):
    any_space = pl.BlockSpec(memory_space=pl.ANY)
    vmem = pltpu.VMEM
    outs = pl.pallas_call(
        kernel,
        out_shape=(
            jax.ShapeDtypeStruct((N, HD), BF),
            jax.ShapeDtypeStruct((N, HD), BF),
            jax.ShapeDtypeStruct((N, HD), BF),
            jax.ShapeDtypeStruct((1, N), F32),
        ),
        in_specs=[any_space] * 23,
        out_specs=[any_space] * 4,
        scratch_shapes=[
            vmem((L, D), BF), vmem((L, D), BF), vmem((D, 3 * HD), BF), vmem((N, D), BF),
            vmem((HD, D), BF), vmem((D, 2 * HD), BF), vmem((HD, D), BF), vmem((D, HD), BF),
            vmem((HD, D), BF), vmem((N, 1, L), F32), vmem((1, N), jnp.int32), vmem((1, D), F32),
            vmem((1, N), F32), vmem((1, D), F32), vmem((1, N), jnp.int32),
            vmem((2, N), jnp.int32), vmem((1, N), F32), vmem((2, N), F32),
            vmem((N, D), BF), vmem((1, D), F32), vmem((N, D), BF), vmem((N, N, HD), BF),
            vmem((N, D), BF), vmem((2 * N, D), BF), vmem((2 * N, D), BF), vmem((N, D), F32),
            vmem((2 * N, D), BF), vmem((2 * N, D), BF), vmem((N, D), BF), vmem((N, N, HD), BF),
            vmem((N, HD), BF), vmem((N, HD), BF), vmem((1, N), F32), vmem((N, HD), BF),
            pltpu.SemaphoreType.DMA((64,)), pltpu.SemaphoreType.DMA((7, N)),
            pltpu.SemaphoreType.DMA((7, N)), pltpu.SemaphoreType.DMA((4,)),
        ],
        compiler_params=pltpu.CompilerParams(
            collective_id=0, has_side_effects=True, vmem_limit_bytes=67_043_328
        ),
    )(
        tokens, key_cache, value_cache, gate_totals, lengths.reshape(1, N),
        attn_gain.reshape(1, D), w_query, w_key, w_value, w_forget.T, forget_bias.reshape(1, N),
        w_attn_out, moe_gain.reshape(1, D), group_ids.T, inner_ids.T,
        group_prob.reshape(1, N), pair_logits.T, w_expert_gate, w_expert_up, w_expert_down, w_dense_in, w_dense_out,
        dense_gate.reshape(1, HD),
    )
    layer, keys, values, gates = pl.pallas_call(
        writer,
        out_shape=[jax.ShapeDtypeStruct(o.shape, o.dtype) for o in outs],
        in_specs=[any_space] * 4,
        out_specs=[any_space] * 4,
        scratch_shapes=[vmem(o.shape, o.dtype) for o in outs] + [pltpu.SemaphoreType.DMA((2, 4))],
        compiler_params=pltpu.CompilerParams(vmem_limit_bytes=67_043_328),
    )(*outs)
    return (layer, keys.reshape(N, 1, HD), values.reshape(N, 1, HD), gates.reshape(N, 1))


def solution(mesh):
    placed = (
        P("ep", "tp"),
        P("ep", "tp", None, None),
        P("ep", "tp", None, None),
        P("ep", "tp", None),
        P("ep"),
        P(),
        P(None, "tp"),
        P(None, "tp"),
        P(None, "tp"),
        P(),
        P(),
        P("tp", None),
        P(),
        P("ep", None),
        P("ep", None),
        P("ep"),
        P("ep", None),
        P("ep", None, "tp"),
        P("ep", None, "tp"),
        P("ep", "tp", None),
        P(None, "tp"),
        P("tp", None),
        P("tp"),
    )
    return jax.shard_map(
        body,
        mesh=mesh,
        in_specs=placed,
        out_specs=(P("ep", "tp"), P("ep", "tp", None), P("ep", "tp", None), P("ep", "tp")),
        check_vma=False,
    )
```
